32 devices in a mesh: sp: 8 (over z, y), dp: 4 (over x, core).
Axes of the slice: x: 2, y: 2, z: 4, core: 2. Of those that a mesh axis runs over, the one named last changes fastest.
Arguments:
- stream: bfloat16 [4, 1024, 2048], P('dp', 'sp'), may hold values from -6 to 6
- query_proj: bfloat16 [4, 1024, 2048], P('dp', 'sp'), may hold values from -6 to 6
- key_proj: bfloat16 [4, 1024, 2048], P('dp', 'sp'), may hold values from -6 to 6
- value_proj: bfloat16 [4, 1024, 2048], P('dp', 'sp'), may hold values from -6 to 6
- out_gate: bfloat16 [4, 1024, 2048], P('dp', 'sp'), may hold values from -6 to 6
- beta_logit: bfloat16 [4, 1024, 16], P('dp', 'sp'), may hold values from -6 to 6
- log_decay: float32 [4, 16, 1024], P('dp', 'sp'), may hold values from -0.8 to 0, as said below
- head_gain: float32 [128], replicated, may hold values from 0.1 to 1.9
- out_proj: bfloat16 [2048, 2048], replicated, may hold values from -0.125 to 0.125
- ffn_gain: float32 [2048], replicated, may hold values from 0.1 to 1.9
- routes: int32 [4, 1024, 2], P('dp', 'sp'), may hold values from 0 to 7, all different within a row; in each aligned block of 128 rows (0 to 127, 128 to 255, ..., all dimensions but the last counted through in order) at most 64 rows name the same one
- route_weight: float32 [4, 1024, 2], P('dp', 'sp'), may hold values from 0.1 to 1
- expert_gate: bfloat16 [8, 2048, 5120], P('sp', None, 'dp'), may hold values from -0.125 to 0.125
- expert_up: bfloat16 [8, 2048, 5120], P('sp', None, 'dp'), may hold values from -0.125 to 0.125
- expert_down: bfloat16 [8, 5120, 2048], P('sp', 'dp'), may hold values from -0.078125 to 0.078125
Outputs:
- result: bfloat16 [4, 1024, 2048], P('dp', 'sp')
The draws below stay inside these ranges and needn't reach their ends.
Inputs may be any that keep to these rules, and one draw needn't show every extreme that they name: `routes`: each row names 2 different experts; within the rows of one device no expert is named more than 64 times, and some devices reach 64. log_decay is never positive.
All inputs are finite; a program needn't handle non-finite values.
Results may differ from the reference program's by a relative error of at most 0.0085.
Values may be sent and summed in bfloat16 or wider, within the bound.
A program may use at most 128 MiB of HBM per device.

```python
import math
import jax
import jax.numpy as jnp
import numpy as np
from jax import lax

D = 2048
MIXER_HEADS = 16
HEAD_DIM = 128
FF = 5120
TOP = 2
BLOCK_LEN = 64
TOK_DEV = 128
SEQUENCE_COUNT = 4
SEQUENCE_LENGTH = 1024
EXPERTS = 8
CAP = 64
N_SP = 8
N_DP = 4


def draw_log_decay(key, part):
    random_split_keys = jax.random.split(jax.random.fold_in(key, 11), 5)
    quick_heads = jax.random.uniform(random_split_keys[0], (1, MIXER_HEADS, 1)) < 0.5
    n_blocks = SEQUENCE_LENGTH // TOK_DEV
    scale_per_block = jnp.exp(jax.random.uniform(random_split_keys[1], (SEQUENCE_COUNT, 1, n_blocks), minval=-0.7, maxval=0.7))
    scale_per_block = jnp.repeat(scale_per_block, TOK_DEV, axis=2)
    random_noise = jax.random.uniform(random_split_keys[2], (SEQUENCE_COUNT, MIXER_HEADS, SEQUENCE_LENGTH), minval=0.25, maxval=1.75)
    baseline_rate = jnp.where(quick_heads, 1.0 / 40.0, 0.5 / SEQUENCE_LENGTH)
    spike_position = jax.random.randint(random_split_keys[3], (SEQUENCE_COUNT, 1, 2), 0, SEQUENCE_LENGTH)
    token_position = jnp.arange(SEQUENCE_LENGTH)[None, None, :, None]
    spike_selected = jnp.any(token_position == spike_position[:, :, None, :], axis=-1)
    spike_magnitude = jax.random.uniform(random_split_keys[4], (SEQUENCE_COUNT, MIXER_HEADS, SEQUENCE_LENGTH), minval=0.22, maxval=0.69)
    return -(baseline_rate * scale_per_block * random_noise) - jnp.where(spike_selected, spike_magnitude, 0.0)


def level_of(rng, dims, cuts, least, largest):
    level = 1.0
    for dim, shards_of in cuts:
        steps = jax.random.uniform(jax.random.fold_in(jax.random.fold_in(rng, 6), dim), (shards_of,), jnp.float32, least / len(cuts), largest / len(cuts))
        level = level * jnp.repeat(jnp.exp(steps), dims[dim] // shards_of).reshape((-1,) + (1,) * (len(dims) - 1 - dim))
    return level


def assign_block(stream_key, own, number, rows, count, top, limit, slope):
    order = jax.random.permutation(stream_key, count)
    heavy_load, usual = portions_of(count, rows * top, limit, slope, True), portions_of(count, rows * top, limit, slope, False)
    places = jnp.arange(count)

    def named(tallies, rotation):
        used = int((tallies > 0).sum())
        fixed = max(1, used // 4)
        shifted = fixed + (places - fixed + rotation * (used - fixed)) % max(1, count - fixed)
        return jnp.zeros((count,), jnp.int32).at[order[jnp.where(places < fixed, places, shifted)]].set(jnp.asarray(tallies, jnp.int32))

    tallies = jnp.where(number % 4 == 0, named(heavy_load, number // 4), named(usual, number - number // 4 - 1))
    mixed = jax.random.permutation(jax.random.fold_in(own, 3), count)
    giver, receiver = mixed[0:count // 2 * 2:2], mixed[1:count // 2 * 2:2]
    room = jnp.minimum(tallies[giver] - 1, limit - tallies[receiver]) // 2
    room = jnp.where((giver == order[0]) | (receiver == order[0]) | (tallies[receiver] == 0), 0, jnp.maximum(room, 0))
    shifted = jax.random.randint(jax.random.fold_in(own, 4), (count // 2,), 0, 1 << 20) % (room + 1)
    tallies = tallies.at[giver].add(-shifted).at[receiver].add(shifted)
    items = jnp.searchsorted(jnp.cumsum(tallies), jnp.arange(rows * top), side="right").astype(jnp.int32)
    grid = items.reshape(top, rows).T
    grid = grid[jax.random.permutation(jax.random.fold_in(own, 1), rows)]
    rotation = jax.random.randint(jax.random.fold_in(own, 2), (rows, 1), 0, top)
    return jnp.take_along_axis(grid, (jnp.arange(top)[None, :] + rotation) % top, axis=1)


def portions_of(amount, total, limit, lean, full):
    weights = [(1 << 20) // math.isqrt(standing ** lean) + 1 for standing in range(1, amount + 1)]
    largest = limit if full else min(limit, max(-(-total // amount), total * weights[0] // sum(weights)))
    least = 1 if total - largest >= amount - 1 else 0
    holding, spare = [largest] + [least] * (amount - 1), total - largest - least * (amount - 1)
    while spare > 0:
        free = [i for i in range(1, amount) if holding[i] < largest] or [i for i in range(1, amount) if holding[i] < limit]
        mass, budget = sum([weights[i] for i in free]), spare
        for i in free:
            more = min(limit - holding[i], max(1, budget * weights[i] // mass), spare)
            holding[i] = holding[i] + more
            spare = spare - more
    return np.array(holding)


def bell_draw(rng, shape, width, most, shards=(), kind=jnp.bfloat16):
    values = jax.random.normal(rng, shape, jnp.float32) * width
    if len(shards) > 0:
        values = level_of(rng, shape, shards, -0.22, 0.18) * values
    return jnp.clip(values, min=-most, max=most).astype(kind)


def setup_inputs(seed: int = 0) -> dict:
    key_of = jax.random.split(jax.random.key(seed), 16)
    stream = bell_draw(key_of[0], (SEQUENCE_COUNT, SEQUENCE_LENGTH, D), 1.0, 6.0, ((0, 4), (1, 8)))
    query_proj = bell_draw(key_of[1], (SEQUENCE_COUNT, SEQUENCE_LENGTH, MIXER_HEADS * HEAD_DIM), 1.0, 6.0, ((0, 4), (1, 8)))
    key_proj = bell_draw(key_of[2], (SEQUENCE_COUNT, SEQUENCE_LENGTH, MIXER_HEADS * HEAD_DIM), 1.0, 6.0, ((0, 4), (1, 8)))
    value_proj = bell_draw(key_of[3], (SEQUENCE_COUNT, SEQUENCE_LENGTH, MIXER_HEADS * HEAD_DIM), 1.0, 6.0, ((0, 4), (1, 8)))
    out_gate = bell_draw(key_of[4], (SEQUENCE_COUNT, SEQUENCE_LENGTH, MIXER_HEADS * HEAD_DIM), 1.0, 6.0, ((0, 4), (1, 8)))
    beta_logit = bell_draw(key_of[5], (SEQUENCE_COUNT, SEQUENCE_LENGTH, MIXER_HEADS), 1.5, 6.0, ((0, 4), (1, 8)))
    log_decay = draw_log_decay(jax.random.fold_in(key_of[15], 71), 0)
    head_gain = jnp.clip(1.0 + 0.18 * jax.random.normal(key_of[7], (HEAD_DIM,), jnp.float32), 0.1, 1.9)
    out_proj = bell_draw(key_of[8], (MIXER_HEADS * HEAD_DIM, D), (MIXER_HEADS * HEAD_DIM) ** -0.5, 0.125)
    ffn_gain = jnp.clip(1.0 + 0.18 * jax.random.normal(key_of[9], (D,), jnp.float32), 0.1, 1.9)
    routes_keys = jax.random.split(jax.random.fold_in(key_of[10], 1), SEQUENCE_COUNT * SEQUENCE_LENGTH // TOK_DEV)
    routes_turns = jax.random.permutation(jax.random.fold_in(key_of[10], 3), SEQUENCE_COUNT * SEQUENCE_LENGTH // TOK_DEV)
    routes = jax.vmap(lambda own, number: assign_block(jax.random.fold_in(key_of[10], 2), own, number, TOK_DEV, EXPERTS, TOP, CAP, 2))(routes_keys, routes_turns).reshape((SEQUENCE_COUNT, SEQUENCE_LENGTH, TOP))
    route_weight = jnp.clip(0.1 + 0.9 * jax.random.uniform(key_of[11], (SEQUENCE_COUNT, SEQUENCE_LENGTH, TOP), jnp.float32) ** level_of(key_of[11], (SEQUENCE_COUNT, SEQUENCE_LENGTH, TOP), ((0, 4), (1, 8)), -0.2, 0.2), 0.1, 1.0)
    expert_gate = bell_draw(key_of[12], (EXPERTS, D, FF), D ** -0.5, 0.125, ((0, 8), (2, 4)))
    expert_up = bell_draw(key_of[13], (EXPERTS, D, FF), D ** -0.5, 0.125, ((0, 8), (2, 4)))
    expert_down = bell_draw(key_of[14], (EXPERTS, FF, D), FF ** -0.5, 0.078125, ((0, 8), (1, 4)))
    return dict(stream=stream, query_proj=query_proj, key_proj=key_proj, value_proj=value_proj, out_gate=out_gate, beta_logit=beta_logit, log_decay=log_decay, head_gain=head_gain, out_proj=out_proj, ffn_gain=ffn_gain, routes=routes, route_weight=route_weight, expert_gate=expert_gate, expert_up=expert_up, expert_down=expert_down)


EPSILON = 1e-06
TOP_PRECISION = lax.Precision.HIGHEST

def unit_rows(matrix):
    return matrix * lax.rsqrt(lax.optimization_barrier(jnp.sum(matrix * matrix, axis=-1, keepdims=True)) + EPSILON)

def delta_blocks(queries, key_rows, values_in, log_rate, strength):
    length, n_heads, key_dim = key_rows.shape
    n_blocks = length // BLOCK_LEN

    def blocked(tensor):
        return tensor.reshape(n_blocks, BLOCK_LEN, n_heads, -1).transpose(0, 2, 1, 3)
    query_blk, key_blk, value_blk = (blocked(queries), blocked(key_rows), blocked(values_in))
    cumulative = jnp.cumsum(log_rate.reshape(n_blocks, BLOCK_LEN, n_heads).transpose(0, 2, 1), axis=-1)
    beta_blk = strength.reshape(n_blocks, BLOCK_LEN, n_heads).transpose(0, 2, 1)
    rows_idx = lax.broadcasted_iota(jnp.int32, (BLOCK_LEN, BLOCK_LEN), 0)
    cols_idx = lax.broadcasted_iota(jnp.int32, (BLOCK_LEN, BLOCK_LEN), 1)
    below_incl = rows_idx >= cols_idx
    strict = rows_idx > cols_idx
    decay_mat = jnp.exp(jnp.where(below_incl, cumulative[..., :, None] - cumulative[..., None, :], -jnp.inf))
    key_beta = key_blk * beta_blk[..., None]
    lower_mat = jnp.where(strict, jnp.einsum('nhid,nhjd->nhij', key_beta, key_blk, precision=TOP_PRECISION) * decay_mat, 0.0)
    system = jnp.eye(BLOCK_LEN, dtype=jnp.float32) + lower_mat
    rhs_cols = jnp.concatenate([value_blk * beta_blk[..., None], key_beta * jnp.exp(cumulative)[..., None]], axis=-1)
    solved = jax.scipy.linalg.solve_triangular(system, rhs_cols, lower=True, unit_diagonal=True)
    value_dim = value_blk.shape[-1]
    update, weight = (solved[..., :value_dim], solved[..., value_dim:])
    inside = jnp.einsum('nhid,nhjd->nhij', query_blk, key_blk, precision=TOP_PRECISION) * decay_mat

    def advance(running_state, inputs):
        query_inner, key_i, update_inner, weight_inner, running_total_inner, inside_i = inputs
        incoming_values = update_inner - jnp.einsum('nli,nif->nlf', weight_inner, running_state, precision=TOP_PRECISION)
        result = jnp.einsum('nli,nif->nlf', query_inner * jnp.exp(running_total_inner)[..., None], running_state, precision=TOP_PRECISION)
        result = result + jnp.einsum('hij,hjv->hiv', inside_i, incoming_values, precision=TOP_PRECISION)
        final_running_total = running_total_inner[:, -1:]
        trailing_key = key_i * jnp.exp(final_running_total - running_total_inner)[..., None]
        running_state = running_state * jnp.exp(final_running_total)[..., None] + jnp.einsum('gbj,gbs->gjs', trailing_key, incoming_values, precision=TOP_PRECISION)
        return (running_state, result)
    zero_state = jnp.zeros((n_heads, key_dim, value_dim), jnp.float32)
    _, results = lax.scan(advance, zero_state, (query_blk, key_blk, update, weight, cumulative, inside))
    return results.transpose(0, 2, 1, 3).reshape(length, n_heads, value_dim)

def mix_sequence(query_in, key_in, value_in, beta_in, decay_in):
    length = query_in.shape[0]
    n_heads = beta_in.shape[1]
    queries = unit_rows(query_in.reshape(length, n_heads, HEAD_DIM).astype(jnp.float32)) * HEAD_DIM ** (-0.5)
    key_rows = unit_rows(key_in.reshape(length, n_heads, HEAD_DIM).astype(jnp.float32))
    values_in = value_in.reshape(length, n_heads, HEAD_DIM).astype(jnp.float32)
    strength = jax.nn.sigmoid(beta_in.astype(jnp.float32))
    log_rate = decay_in.astype(jnp.float32).T

    def two_ways(tensor):
        return jnp.concatenate([tensor, tensor[::-1]], axis=1)
    reads = delta_blocks(two_ways(queries), two_ways(key_rows), two_ways(values_in), two_ways(log_rate), two_ways(strength))
    summed = reads[:, :n_heads] + reads[::-1, n_heads:]
    return summed.astype(jnp.bfloat16).reshape(length, n_heads * HEAD_DIM)

def reference(stream, query_proj, key_proj, value_proj, out_gate, beta_logit, log_decay, head_gain, out_proj, ffn_gain, routes, route_weight, expert_gate, expert_up, expert_down):

    def one_sequence(inputs):
        return mix_sequence(*inputs)
    mixed = lax.map(one_sequence, (query_proj, key_proj, value_proj, beta_logit, log_decay))
    model_width = stream.shape[2]
    n_tokens = stream.shape[0] * stream.shape[1]
    per_head = mixed.reshape(n_tokens, MIXER_HEADS, HEAD_DIM).astype(jnp.float32)
    normed_heads = per_head * lax.rsqrt(lax.optimization_barrier(jnp.mean(per_head * per_head, axis=-1, keepdims=True)) + EPSILON) * head_gain
    gated = (normed_heads.reshape(n_tokens, -1) * jax.nn.silu(out_gate.reshape(n_tokens, -1).astype(jnp.float32))).astype(jnp.bfloat16)
    resid = stream.reshape(n_tokens, model_width).astype(jnp.float32) + jnp.dot(gated.astype(jnp.float32), out_proj.astype(jnp.float32), preferred_element_type=jnp.float32)
    ffn_in = (resid * lax.rsqrt(lax.optimization_barrier(jnp.mean(resid * resid, axis=-1, keepdims=True)) + EPSILON) * ffn_gain).astype(jnp.bfloat16)
    n_rows = N_SP * N_DP * CAP
    flat_routes = routes.reshape(n_tokens, TOP)
    flat_weight = route_weight.reshape(n_tokens, TOP)
    group_width = FF // N_DP

    def one_expert(index):
        hits = flat_routes == index
        member = jnp.any(hits, axis=1).astype(jnp.int32)
        order = jnp.argsort(1 - member, stable=True)[:n_rows].astype(jnp.int32)
        picked = ffn_in[order]
        share = lax.optimization_barrier(jnp.sum(jnp.where(hits, flat_weight, 0.0), axis=1))[order]
        gate_act = jnp.dot(picked.astype(jnp.float32), expert_gate[index].astype(jnp.float32), preferred_element_type=jnp.float32)
        up_act = jnp.dot(picked.astype(jnp.float32), expert_up[index].astype(jnp.float32), preferred_element_type=jnp.float32)
        hidden = (jax.nn.silu(gate_act) * up_act).astype(jnp.bfloat16)
        pieces = jnp.einsum('rpf,pfd->prd', hidden.reshape(n_rows, N_DP, group_width).astype(jnp.float32), expert_down[index].reshape(N_DP, group_width, model_width).astype(jnp.float32))
        rounded = lax.optimization_barrier(pieces.astype(jnp.bfloat16))
        expert_out = lax.optimization_barrier(jnp.sum(rounded.astype(jnp.float32), axis=0)).astype(jnp.bfloat16)
        return (order, expert_out.astype(jnp.float32) * share[:, None])
    orders, contribs = lax.map(one_expert, jnp.arange(EXPERTS, dtype=jnp.int32))
    routed = jax.ops.segment_sum(contribs.reshape(-1, model_width), orders.reshape(-1), num_segments=n_tokens)
    return (resid + routed).astype(jnp.bfloat16).reshape(stream.shape)
```

```python
import functools

import jax
import jax.numpy as jnp
from jax import lax
from jax.experimental import pallas as pl
from jax.experimental.pallas import tpu as pltpu
from jax.sharding import PartitionSpec as P

HEAD_DIM = 128
CHUNK = 128
CORES = 2
EPSILON = 1e-06
MESH = pl.DeviceIdType.MESH


def mm(a, b):
    return lax.dot_general(a, b, (((1,), (0,)), ((), ())), preferred_element_type=jnp.float32)


def mm_t(a, b):
    return lax.dot_general(a, b, (((1,), (1,)), ((), ())), preferred_element_type=jnp.float32)


def mixer_kernel(
    n_heads, q_ref, k_ref, v_ref, beta_ref, rate_ref, out_ref, upd, wq, ins, trail, reads, state
):
    n_chunks = q_ref.shape[0] // CHUNK
    bf = jnp.bfloat16
    row = lax.broadcasted_iota(jnp.int32, (CHUNK, CHUNK), 0)
    col = lax.broadcasted_iota(jnp.int32, (CHUNK, CHUNK), 1)
    chains = [(head, way) for head in range(n_heads) for way in range(2)]

    def prepare(c, carry):
        rows = pl.ds(pl.multiple_of(c * CHUNK, CHUNK), CHUNK)
        apart = row ^ col
        eye = row == col
        todo = []
        for head in range(n_heads):
            lanes = slice(head * HEAD_DIM, (head + 1) * HEAD_DIM)
            q = q_ref[rows, lanes].astype(jnp.float32)
            k = k_ref[rows, lanes].astype(jnp.float32)
            v = v_ref[rows, lanes]
            qn = q * (
                lax.rsqrt(jnp.sum(q * q, axis=1, keepdims=True) + EPSILON) * HEAD_DIM ** (-0.5)
            )
            kn = k * lax.rsqrt(jnp.sum(k * k, axis=1, keepdims=True) + EPSILON)
            kn_t = kn.T
            kb = kn.astype(bf)
            gram = mm_t(kb, kb)
            cross = mm_t(qn.astype(bf), kb)
            beta_row = jax.nn.sigmoid(beta_ref[c, head : head + 1, :].astype(jnp.float32))
            rate_row = rate_ref[c, head : head + 1, :]
            beta_col = jnp.sum(jnp.where(eye, beta_row, 0.0), axis=1, keepdims=True)
            rate_col = jnp.sum(jnp.where(eye, rate_row, 0.0), axis=1, keepdims=True)
            total = jnp.sum(rate_row, axis=1, keepdims=True)
            for way in range(2):
                incl = (row >= col) if way == 0 else (row <= col)
                incl_t = (row <= col) if way == 0 else (row >= col)
                strict = (row > col) if way == 0 else (row < col)
                kept = jnp.where(incl, rate_row, 0.0)
                high = kept.astype(bf)
                low = (kept - high.astype(jnp.float32)).astype(bf)
                after = strict.astype(jnp.float32).astype(bf)
                decay = jnp.where(incl, jnp.exp(mm(high, after) + mm(low, after)), 0.0)
                run_col = jnp.sum(kept, axis=1, keepdims=True)
                run_row = jnp.sum(jnp.where(incl_t, rate_col, 0.0), axis=0, keepdims=True)
                lower = jnp.where(strict, beta_col * gram * decay, 0.0)
                inverse = jnp.where(eye, 1.0, jnp.where(apart == 1, -lower, 0.0))
                slot = (head * 2 + way) * n_chunks + c
                ins[slot] = (cross * decay).astype(bf)
                trail[slot] = (kn_t * jnp.exp(total - run_row)).astype(bf)
                wq[slot, CHUNK:, :] = (qn * jnp.exp(run_col)).astype(bf)
                todo.append([slot, lower, inverse, beta_row, jnp.exp(run_row), v, kb])
        level = 1
        while (1 << level) < CHUNK:
            firsts = []
            for item in todo:
                now = item[2].astype(bf)
                part = jnp.where((apart >> level) == 1, item[1], 0.0).astype(bf)
                firsts.append((now, mm(now, part).astype(bf)))
            for item, (now, first) in zip(todo, firsts):
                item[2] = item[2] - mm(first, now)
            level += 1
        for slot, _, inverse, beta_row, grown, v, kb in todo:
            scaled = inverse * beta_row
            upd[slot] = mm(scaled.astype(bf), v)
            wq[slot, :CHUNK, :] = mm((scaled * grown).astype(bf), kb).astype(bf)
        return carry

    lax.fori_loop(0, n_chunks, prepare, 0)
    state[...] = jnp.zeros_like(state)

    def advance(step, carry):
        work = []
        for index, (head, way) in enumerate(chains):
            c = step if way == 0 else n_chunks - 1 - step
            slot = index * n_chunks + c
            work.append((index, head, way, c, slot, mm(wq[slot], state[index].astype(bf))))
        fresh = []
        for index, head, way, c, slot, both in work:
            fresh.append((upd[slot] - both[:CHUNK]).astype(bf))
        for (index, head, way, c, slot, both), new in zip(work, fresh):
            total = jnp.sum(rate_ref[c, head : head + 1, :], axis=1, keepdims=True)
            state[index] = state[index] * jnp.exp(total) + mm(trail[slot], new)
        for (index, head, way, c, slot, both), new in zip(work, fresh):
            reads[slot] = both[CHUNK:] + mm(ins[slot], new)
        return carry

    lax.fori_loop(0, n_chunks, advance, 0)

    def finish(c, carry):
        rows = pl.ds(pl.multiple_of(c * CHUNK, CHUNK), CHUNK)
        for head in range(n_heads):
            lanes = slice(head * HEAD_DIM, (head + 1) * HEAD_DIM)
            one = reads[head * 2 * n_chunks + c]
            two = reads[(head * 2 + 1) * n_chunks + c]
            out_ref[rows, lanes] = (one + two).astype(bf)
        return carry

    lax.fori_loop(0, n_chunks, finish, 0)


def mix(q, k, v, beta, rate):
    length, width = q.shape
    n_heads = width // HEAD_DIM
    n_chunks = length // CHUNK
    slots = 2 * n_heads * n_chunks
    vmem = pl.BlockSpec(memory_space=pltpu.VMEM)
    return pl.pallas_call(
        functools.partial(mixer_kernel, n_heads),
        out_shape=jax.ShapeDtypeStruct((length, width), jnp.bfloat16),
        in_specs=[vmem] * 5,
        out_specs=vmem,
        scratch_shapes=[
            pltpu.VMEM((slots, CHUNK, HEAD_DIM), jnp.float32),
            pltpu.VMEM((slots, 2 * CHUNK, HEAD_DIM), jnp.bfloat16),
            pltpu.VMEM((slots, CHUNK, CHUNK), jnp.bfloat16),
            pltpu.VMEM((slots, HEAD_DIM, CHUNK), jnp.bfloat16),
            pltpu.VMEM((slots, CHUNK, HEAD_DIM), jnp.float32),
            pltpu.VMEM((2 * n_heads, HEAD_DIM, HEAD_DIM), jnp.float32),
        ],
        compiler_params=pltpu.CompilerParams(vmem_limit_bytes=40 * 1024 * 1024),
        cost_estimate=pl.CostEstimate(
            flops=40 * slots * CHUNK**3, bytes_accessed=8 * length * width, transcendentals=0
        ),
        name="mixer",
    )(q, k, v, beta, rate)


ANY = pl.BlockSpec(memory_space=pl.ANY)


def exchange_kernel(n, count, take, put, *refs):
    sources, targets = refs[:count], refs[count : 2 * count]
    send_sem, recv_sem, own_sem = refs[2 * count :]
    me = lax.axis_index("sp")
    barrier = pltpu.get_barrier_semaphore()
    for hop in range(1, n):
        pl.semaphore_signal(
            barrier, inc=1, device_id={"sp": lax.rem(me + hop, n)}, device_id_type=MESH
        )
    pl.semaphore_wait(barrier, n - 1)
    copies = []
    for hop in range(1, n):
        peer = lax.rem(me + hop, n)
        for i in range(count):
            copy = pltpu.make_async_remote_copy(
                src_ref=take(sources[i], peer),
                dst_ref=put(targets[i], me),
                send_sem=send_sem.at[i, hop - 1],
                recv_sem=recv_sem.at[i, hop - 1],
                device_id={"sp": peer},
                device_id_type=MESH,
            )
            copy.start()
            copies.append(copy)
    for i in range(count):
        copy = pltpu.make_async_copy(
            take(sources[i], me), put(targets[i], me), own_sem.at[i]
        )
        copy.start()
        copies.append(copy)
    for copy in copies:
        copy.wait()


def exchange(n, arrays, shapes, take, put, collective_id, name):
    count = len(arrays)
    return pl.pallas_call(
        functools.partial(exchange_kernel, n, count, take, put),
        out_shape=[jax.ShapeDtypeStruct(s, a.dtype) for s, a in zip(shapes, arrays)],
        in_specs=[ANY] * count,
        out_specs=[ANY] * count,
        scratch_shapes=[
            pltpu.SemaphoreType.DMA((count, n - 1)),
            pltpu.SemaphoreType.DMA((count, n - 1)),
            pltpu.SemaphoreType.DMA((count,)),
        ],
        compiler_params=pltpu.CompilerParams(collective_id=collective_id, has_side_effects=True),
        name=name,
    )(*arrays)


def lead_block(ref, index):
    return ref.at[index]


def row_block(rows, ref, index):
    return ref.at[pl.ds(pl.multiple_of(index * rows, rows), rows), :]


def lane_block(lanes, ref, index):
    return ref.at[:, pl.ds(pl.multiple_of(index * lanes, lanes), lanes)]


def spread_kernel(
    n, n_dp, x_ref, out_ref, own_sem, a_send, a_recv, b_send, b_recv, c_send, c_recv
):
    me, mine = lax.axis_index("sp"), lax.axis_index("dp")
    chips = n_dp // CORES
    chip, core = mine // CORES, lax.rem(mine, CORES)
    sibling = chip * CORES + (1 - core)
    barrier = pltpu.get_barrier_semaphore()
    for hop in range(1, n):
        pl.semaphore_signal(
            barrier, inc=1, device_id={"sp": lax.rem(me + hop, n)}, device_id_type=MESH
        )
    for turn in range(1, chips):
        other = lax.rem(chip + turn, chips) * CORES + core
        pl.semaphore_signal(barrier, inc=1, device_id={"dp": other}, device_id_type=MESH)
    pl.semaphore_signal(barrier, inc=1, device_id={"dp": sibling}, device_id_type=MESH)
    pl.semaphore_wait(barrier, n - 1 + chips - 1 + 1)

    own = pltpu.make_async_copy(x_ref.at[me], out_ref.at[mine, me], own_sem)
    own.start()
    first = [None]
    for hop in range(1, n):
        peer = lax.rem(me + hop, n)
        copy = pltpu.make_async_remote_copy(
            src_ref=x_ref.at[peer],
            dst_ref=out_ref.at[mine, me],
            send_sem=a_send.at[hop - 1],
            recv_sem=a_recv.at[hop - 1],
            device_id={"sp": peer},
            device_id_type=MESH,
        )
        copy.start()
        first.append(copy)
    across, beside = {}, []
    for hop in range(n):
        origin = lax.rem(me + n - hop, n)
        if hop == 0:
            block = x_ref.at[me]
        else:
            first[hop].wait_recv()
            block = out_ref.at[mine, origin]
        for turn in range(1, chips):
            other = lax.rem(chip + turn, chips) * CORES + core
            copy = pltpu.make_async_remote_copy(
                src_ref=block,
                dst_ref=out_ref.at[mine, origin],
                send_sem=b_send.at[turn - 1, hop],
                recv_sem=b_recv.at[turn - 1, hop],
                device_id={"dp": other},
                device_id_type=MESH,
            )
            copy.start()
            across[turn, hop] = copy
        copy = pltpu.make_async_remote_copy(
            src_ref=block,
            dst_ref=out_ref.at[mine, origin],
            send_sem=c_send.at[0, hop],
            recv_sem=c_recv.at[0, hop],
            device_id={"dp": sibling},
            device_id_type=MESH,
        )
        copy.start()
        beside.append(copy)
    for hop in range(n):
        origin = lax.rem(me + n - hop, n)
        for turn in range(1, chips):
            across[turn, hop].wait_recv()
            giver = lax.rem(chip + chips - turn, chips) * CORES + core
            copy = pltpu.make_async_remote_copy(
                src_ref=out_ref.at[giver, origin],
                dst_ref=out_ref.at[giver, origin],
                send_sem=c_send.at[turn, hop],
                recv_sem=c_recv.at[turn, hop],
                device_id={"dp": sibling},
                device_id_type=MESH,
            )
            copy.start()
            beside.append(copy)
    own.wait()
    for hop in range(1, n):
        first[hop].wait_send()
    for copy in across.values():
        copy.wait_send()
    for copy in beside:
        copy.wait()


def spread(n, n_dp, x, collective_id):
    chips = n_dp // CORES
    dma = pltpu.SemaphoreType.DMA
    return pl.pallas_call(
        functools.partial(spread_kernel, n, n_dp),
        out_shape=jax.ShapeDtypeStruct((n_dp,) + x.shape, x.dtype),
        in_specs=[ANY],
        out_specs=ANY,
        scratch_shapes=[
            dma,
            dma((n - 1,)),
            dma((n - 1,)),
            dma((max(chips - 1, 1), n)),
            dma((max(chips - 1, 1), n)),
            dma((chips, n)),
            dma((chips, n)),
        ],
        compiler_params=pltpu.CompilerParams(collective_id=collective_id, has_side_effects=True),
        name="spread",
    )(x)


def expert_part(rows, gate_local, up_local, down_local):
    gate_act = jnp.dot(rows, gate_local, preferred_element_type=jnp.float32)
    up_act = jnp.dot(rows, up_local, preferred_element_type=jnp.float32)
    hidden = (jax.nn.silu(gate_act) * up_act).astype(jnp.bfloat16)
    return jnp.dot(hidden, down_local, preferred_element_type=jnp.float32)


def body(
    stream,
    query_proj,
    key_proj,
    value_proj,
    out_gate,
    beta_logit,
    log_decay,
    head_gain,
    out_proj,
    ffn_gain,
    routes,
    route_weight,
    expert_gate,
    expert_up,
    expert_down,
):
    n_sp = lax.axis_size("sp")
    n_dp = lax.axis_size("dp")
    tok_here = stream.shape[1]
    heads_here = log_decay.shape[1]
    length = log_decay.shape[2]
    width = heads_here * HEAD_DIM
    beta_out = beta_logit[0].T.astype(jnp.float32).reshape(n_sp, heads_here, tok_here)
    beta_out = jnp.pad(beta_out, ((0, 0), (0, -heads_here % 8), (0, 0)))
    projections = exchange(
        n_sp,
        (query_proj[0], key_proj[0], value_proj[0]),
        ((length, width),) * 3,
        functools.partial(lane_block, width),
        functools.partial(row_block, tok_here),
        1,
        "to_heads",
    )
    (beta_in,) = exchange(
        n_sp, (beta_out,), (beta_out.shape,), lead_block, lead_block, 2, "to_heads_beta"
    )
    pieces = tok_here // CHUNK
    beta_in = beta_in[:, :heads_here].reshape(n_sp, heads_here, pieces, CHUNK)
    beta_in = beta_in.transpose(0, 2, 1, 3).reshape(n_sp * pieces, heads_here, CHUNK)
    rate_in = log_decay[0].reshape(heads_here, length // CHUNK, CHUNK).transpose(1, 0, 2)
    mixed = mix(*projections, beta_in, rate_in)
    (tokens_view,) = exchange(
        n_sp,
        (mixed,),
        ((tok_here, n_sp * width),),
        functools.partial(row_block, tok_here),
        functools.partial(lane_block, width),
        3,
        "to_tokens",
    )
    tok_count = stream.shape[1]
    model_width = stream.shape[2]
    n_heads = tokens_view.shape[1] // HEAD_DIM
    per_head = tokens_view.astype(jnp.float32).reshape(tok_count, n_heads, HEAD_DIM)
    normed_heads = (
        per_head
        * lax.rsqrt(jnp.mean(per_head * per_head, axis=-1, keepdims=True) + EPSILON)
        * head_gain
    )
    gated = (
        normed_heads.reshape(tok_count, -1) * jax.nn.silu(out_gate[0].astype(jnp.float32))
    ).astype(jnp.bfloat16)
    resid = stream[0].astype(jnp.float32) + jnp.dot(
        gated, out_proj, preferred_element_type=jnp.float32
    )
    ffn_in = (
        resid * lax.rsqrt(jnp.mean(resid * resid, axis=-1, keepdims=True) + EPSILON) * ffn_gain
    ).astype(jnp.bfloat16)
    top_count = routes.shape[2]
    capacity = tok_count * top_count * 2 // n_sp
    flat_routes = routes.reshape(-1)
    expert_ids = lax.broadcasted_iota(jnp.int32, (1, n_sp), 1)
    chosen = (flat_routes[:, None] == expert_ids).astype(jnp.int32)
    earlier = jnp.cumsum(chosen, axis=0) - chosen
    slot_ids = flat_routes * capacity + jnp.sum(earlier * chosen, axis=1)
    slot_grid = lax.broadcasted_iota(jnp.int32, (n_sp * capacity, 1), 0)
    placing = (
        (slot_grid == slot_ids[None, :])
        .astype(jnp.int32)
        .reshape(n_sp * capacity, tok_count, top_count)
    )
    placing = jnp.sum(placing, axis=2).astype(jnp.bfloat16)
    outgoing = jnp.dot(placing, ffn_in, preferred_element_type=jnp.float32).astype(jnp.bfloat16)
    outgoing = outgoing.reshape(n_sp, capacity, model_width)
    gate_local = expert_gate[0]
    up_local = expert_up[0]
    down_local = expert_down[0]
    piece = spread(n_sp, n_dp, outgoing, 4)
    flat_rows = piece.reshape(-1, model_width)
    partial_value = expert_part(flat_rows, gate_local, up_local, down_local).reshape(
        n_dp * n_sp, capacity, model_width
    )
    summed = lax.psum_scatter(
        partial_value.astype(jnp.bfloat16), "dp", scatter_dimension=0, tiled=True
    )
    (returned,) = exchange(
        n_sp, (summed,), (summed.shape,), lead_block, lead_block, 5, "expert_return"
    )
    picked = returned.reshape(n_sp * capacity, model_width)[slot_ids]
    picked = picked.reshape(tok_count, top_count, model_width).astype(jnp.float32)
    routed = jnp.sum(picked * route_weight[0][..., None], axis=1)
    return (resid + routed).astype(jnp.bfloat16)[None]


def solution(mesh):
    return jax.shard_map(
        body,
        mesh=mesh,
        in_specs=(
            P("dp", "sp", None),
            P("dp", "sp", None),
            P("dp", "sp", None),
            P("dp", "sp", None),
            P("dp", "sp", None),
            P("dp", "sp", None),
            P("dp", "sp", None),
            P(),
            P(),
            P(),
            P("dp", "sp", None),
            P("dp", "sp", None),
            P("sp", None, "dp"),
            P("sp", None, "dp"),
            P("sp", "dp", None),
        ),
        out_specs=P("dp", "sp", None),
        check_vma=False,
    )
```
